32 devices in a mesh: ep: 8 (over z, core), tp: 4 (over y, x).
Axes of the slice: x: 2, y: 2, z: 4, core: 2. Of those that a mesh axis runs over, the one named last changes fastest.
Arguments:
- probe_preactivations: bfloat16 [4096, 2048], P('ep', 'tp'), may hold values from -6 to 6
- rightward_retain_scores: bfloat16 [4096, 2048], P('ep', 'tp'), may hold values from -5.5 to 5.5
- leftward_retain_scores: bfloat16 [4096, 2048], P('ep', 'tp'), may hold values from -5.5 to 5.5
- payload_vectors: bfloat16 [4096, 2048], P('ep', 'tp'), may hold values from -6 to 6
- retain_minimum_bounds: float32 [2, 2048], P(None, 'tp'), may hold values from 0.88 to 1
- extra_shrink_spikes: float32 [16, 4096], P('tp', 'ep'), may hold values from -0.7 to 0
- mixer_rescale_factor: float32 [2048], P('tp'), may hold values from 0.1 to 1.9
- mixer_emit_matrix: bfloat16 [2048, 2048], P('tp'), may hold values from -0.1875 to 0.1875
- specialist_arriving_tokens: bfloat16 [1024, 2048], P('ep'), may hold values from -6 to 6
- specialist_rescale_factor: float32 [2048], replicated, may hold values from 0.1 to 1.9
- routed_specialist_ids: int32 [1024, 2], P('ep'), may hold values from 0 to 7, all different within a row; in each aligned block of 128 rows (0 to 127, 128 to 255, ...) at most 64 rows name the same one
- routed_specialist_shares: float32 [1024, 2], P('ep'), may hold values from 0.1 to 1
- specialist_switch_matrix: bfloat16 [8, 2048, 3584], P('ep', None, 'tp'), may hold values from -0.125 to 0.125
- specialist_widen_matrix: bfloat16 [8, 2048, 3584], P('ep', None, 'tp'), may hold values from -0.125 to 0.125
- specialist_shrink_matrix: bfloat16 [8, 3584, 2048], P('ep', 'tp'), may hold values from -0.125 to 0.125
Outputs:
- mixed_a: bfloat16 [4096, 2048], P('ep', 'tp')
- mixed_b: bfloat16 [1024, 2048], P('ep', 'tp')
The draws below stay inside these ranges and needn't reach their ends.
Inputs may be any that keep to these rules, and one draw needn't show every extreme that they name: `routed_specialist_ids`: each row names 2 different experts; within the rows of one index of ep no expert is named by more than 64 rows, and in every draw some expert is named by exactly 64 rows of some index.
All inputs are finite; a program needn't handle non-finite values.
Results may differ from the reference program's by a relative error of at most 0.015.
Values may be sent and summed in bfloat16 or wider, within the bound.
A program may use at most 64 MiB of HBM per device.

```python
import math
import jax
import jax.numpy as jnp
import numpy as np
from jax import lax

D = 2048
MIXER_STREAMS = 16
DK = 128
DE = 3584
TOP_K = 2
SPAN = 32
TOK_A = 512
TOK_B = 128
DV = 128
F = 2048
SEQ = 4096
ROWS_B = 1024
EXPERTS = 8
CAP = 64
N_EP = 8
N_TP = 4


def forget_draw(key):
    noise_key, offset_key = jax.random.split(key)
    noise = jnp.clip(jax.random.normal(noise_key, (SEQ, F), jnp.float32), -4.0, 4.0)
    offsets = jax.random.uniform(offset_key, (SEQ // TOK_A, 1, F), jnp.float32, -1.5, 1.5)
    shifted = noise.reshape(SEQ // TOK_A, TOK_A, F) + offsets
    return shifted.reshape(SEQ, F).astype(jnp.bfloat16)


def draw_rightward_retain_scores(key, part):
    return forget_draw(jax.random.fold_in(key, 11))


def draw_leftward_retain_scores(key, part):
    return forget_draw(jax.random.fold_in(key, 12))


def draw_retain_minimum_bounds(key, part):
    kind_key, slow_key, fast_key = jax.random.split(jax.random.fold_in(key, 21), 3)
    slow_head = jax.random.randint(kind_key, (2, MIXER_STREAMS, 1), 0, 2) > 0
    slow_gap = jax.random.uniform(slow_key, (2, MIXER_STREAMS, DK), jnp.float32, 0.5, 2.0) / SEQ
    fast_gap = jnp.exp(jax.random.uniform(fast_key, (2, MIXER_STREAMS, DK), jnp.float32, -3.2, -2.13))
    chosen_gap = jnp.where(slow_head, slow_gap, fast_gap)
    return (1.0 - chosen_gap).reshape(2, F).astype(jnp.float32)


def draw_extra_shrink_spikes(key, part):
    where_key, depth_key = jax.random.split(jax.random.fold_in(key, 31))
    struck = jax.random.randint(where_key, (MIXER_STREAMS, SEQ), 0, SEQ) < 6
    depth = jnp.log(1.0 - jax.random.uniform(depth_key, (MIXER_STREAMS, SEQ), jnp.float32, 0.2, 0.5))
    return jnp.where(struck, depth, 0.0).astype(jnp.float32)


def strengthened(entries, key, source, target, shards_of, factor):
    def block_of(dim):
        return (jnp.arange(entries.shape[dim]) // (entries.shape[dim] // shards_of)).reshape((-1,) + (1,) * (entries.ndim - 1 - dim))

    first = jax.random.permutation(key, shards_of)[block_of(target)]
    second = (block_of(target) + shards_of // 2) % shards_of
    return jnp.where((block_of(source) == first) | (block_of(source) == second), factor * entries, entries)


def steps_of(own_key, dims, cuts, smallest, top_value):
    def one(axis_at, blocks):
        draws = jax.random.uniform(jax.random.fold_in(jax.random.fold_in(own_key, 6), axis_at), (blocks,), jnp.float32, smallest / len(cuts), top_value / len(cuts))
        return jnp.repeat(jnp.exp(draws), dims[axis_at] // blocks).reshape((-1,) + (1,) * (len(dims) - axis_at - 1))

    gain = one(*cuts[0])
    for cut in cuts[1:]:
        gain = gain * one(*cut)
    return gain


def deal_out(rng, own, number, rows, number_of, top, limit, skew):
    order = jax.random.permutation(rng, number_of)
    packed, usual = shares(number_of, rows * top, limit, skew, True), shares(number_of, rows * top, limit, skew, False)
    places = jnp.arange(number_of)

    def named(sizes, rotation):
        used = int((sizes > 0).sum())
        fixed = max(1, used // 4)
        moved = fixed + (places - fixed + rotation * (used - fixed)) % max(1, number_of - fixed)
        return jnp.zeros((number_of,), jnp.int32).at[order[jnp.where(places < fixed, places, moved)]].set(jnp.asarray(sizes, jnp.int32))

    sizes = jnp.where(number % 4 == 0, named(packed, number // 4), named(usual, number - number // 4 - 1))
    mixed = jax.random.permutation(jax.random.fold_in(own, 3), number_of)
    giver, sink = mixed[0:number_of // 2 * 2:2], mixed[1:number_of // 2 * 2:2]
    slack = jnp.minimum(sizes[giver] - 1, limit - sizes[sink]) // 2
    slack = jnp.where((giver == order[0]) | (sink == order[0]) | (sizes[sink] == 0), 0, jnp.maximum(slack, 0))
    moved = jax.random.randint(jax.random.fold_in(own, 4), (number_of // 2,), 0, 1 << 20) % (slack + 1)
    sizes = sizes.at[giver].add(-moved).at[sink].add(moved)
    items = jnp.searchsorted(jnp.cumsum(sizes), jnp.arange(rows * top), side="right").astype(jnp.int32)
    table = items.reshape(top, rows).T
    table = table[jax.random.permutation(jax.random.fold_in(own, 1), rows)]
    rotation = jax.random.randint(jax.random.fold_in(own, 2), (rows, 1), 0, top)
    return jnp.take_along_axis(table, (jnp.arange(top)[None, :] + rotation) % top, axis=1)


def shares(number_of, total, most, lean, full):
    weights = [(1 << 20) // math.isqrt(standing ** lean) + 1 for standing in range(1, number_of + 1)]
    largest = most if full else min(most, max(-(-total // number_of), total * weights[0] // sum(weights)))
    least = 1 if total - largest >= number_of - 1 else 0
    holding, rest = [largest] + [least] * (number_of - 1), total - largest - least * (number_of - 1)
    while rest > 0:
        candidates = [i for i in range(1, number_of) if holding[i] < largest] or [i for i in range(1, number_of) if holding[i] < most]
        mass, left = sum([weights[i] for i in candidates]), rest
        for i in candidates:
            more = min(most - holding[i], max(1, left * weights[i] // mass), rest)
            holding[i] = holding[i] + more
            rest = rest - more
    return np.array(holding)


def gaussian(own_key, dims, deviation, most, cuts=(), kind=jnp.bfloat16):
    entries = jax.random.normal(own_key, dims, jnp.float32) * deviation
    if len(cuts) > 0:
        entries = steps_of(own_key, dims, cuts, -0.22, 0.18) * entries
    return jnp.clip(entries, min=-most, max=most).astype(kind)


def gaussian_with(key, shape, deviation, most, cuts, heavy, kind=jnp.bfloat16):
    result = deviation * jax.random.normal(key, shape, jnp.float32)
    if cuts:
        result = result * steps_of(key, shape, cuts, -0.22, 0.18)
    return jnp.clip(strengthened(result, jax.random.fold_in(key, 3), *heavy), -most, most).astype(kind)


def setup_inputs(seed: int = 0) -> dict:
    keys = jax.random.split(jax.random.key(seed), 16)
    probe_preactivations = gaussian(keys[0], (SEQ, F), 1.0, 6.0, ((0, 8), (1, 4)))
    rightward_retain_scores = draw_rightward_retain_scores(jax.random.fold_in(keys[15], 71), 0)
    leftward_retain_scores = draw_leftward_retain_scores(jax.random.fold_in(keys[15], 71), 0)
    payload_vectors = gaussian(keys[3], (SEQ, D), 1.0, 6.0, ((0, 8), (1, 4)))
    retain_minimum_bounds = draw_retain_minimum_bounds(jax.random.fold_in(keys[15], 71), 0)
    extra_shrink_spikes = draw_extra_shrink_spikes(jax.random.fold_in(keys[15], 71), 0)
    mixer_rescale_factor = jnp.clip(1.0 + 0.18 * jax.random.normal(keys[6], (D,), jnp.float32), 0.1, 1.9)
    mixer_emit_matrix = gaussian_with(keys[7], (D, D), D ** -0.5, 0.1875, ((0, 4),), (0, 1, 4, 2.0))
    specialist_arriving_tokens = gaussian(keys[8], (ROWS_B, D), 1.0, 6.0, ((0, 8),))
    specialist_rescale_factor = jnp.clip(1.0 + 0.18 * jax.random.normal(keys[9], (D,), jnp.float32), 0.1, 1.9)
    routed_specialist_ids_keys = jax.random.split(jax.random.fold_in(keys[10], 1), ROWS_B // TOK_B)
    routed_specialist_ids_turns = jax.random.permutation(jax.random.fold_in(keys[10], 3), ROWS_B // TOK_B)
    routed_specialist_ids = jax.vmap(lambda own, number: deal_out(jax.random.fold_in(keys[10], 2), own, number, TOK_B, EXPERTS, TOP_K, CAP, 2))(routed_specialist_ids_keys, routed_specialist_ids_turns).reshape((ROWS_B, TOP_K))
    routed_specialist_shares = jnp.clip(0.1 + 0.9 * jax.random.uniform(keys[11], (ROWS_B, TOP_K), jnp.float32) ** steps_of(keys[11], (ROWS_B, TOP_K), ((0, 8),), -0.2, 0.2), 0.1, 1.0)
    specialist_switch_matrix = gaussian(keys[12], (EXPERTS, D, DE), D ** -0.5, 0.125, ((0, 8), (2, 4)))
    specialist_widen_matrix = gaussian(keys[13], (EXPERTS, D, DE), D ** -0.5, 0.125, ((0, 8), (2, 4)))
    specialist_shrink_matrix = gaussian_with(keys[14], (EXPERTS, DE, D), DE ** -0.5, 0.125, ((0, 8), (1, 4)), (1, 2, 4, 2.0))
    return {"probe_preactivations": probe_preactivations, "rightward_retain_scores": rightward_retain_scores, "leftward_retain_scores": leftward_retain_scores, "payload_vectors": payload_vectors, "retain_minimum_bounds": retain_minimum_bounds, "extra_shrink_spikes": extra_shrink_spikes, "mixer_rescale_factor": mixer_rescale_factor, "mixer_emit_matrix": mixer_emit_matrix, "specialist_arriving_tokens": specialist_arriving_tokens, "specialist_rescale_factor": specialist_rescale_factor, "routed_specialist_ids": routed_specialist_ids, "routed_specialist_shares": routed_specialist_shares, "specialist_switch_matrix": specialist_switch_matrix, "specialist_widen_matrix": specialist_widen_matrix, "specialist_shrink_matrix": specialist_shrink_matrix}


EPS = 1e-06
NEG_BIG = -1e+30
HIGH_PRECISION = lax.Precision.HIGHEST

def recurrence(query_heads, key_gate, v_heads, shrink_exponent, state_in):
    channel_group_count, length, _ = query_heads.shape
    block_count = length // SPAN

    def blocks(tensor):
        return jnp.moveaxis(tensor.reshape(channel_group_count, block_count, SPAN, tensor.shape[-1]), 1, 0)
    lower_tri = jnp.tril(jnp.ones((SPAN, SPAN), dtype=bool))[:, :, None]

    def advance(carried_state, pieces):
        query_block, key_block, value_block, l_blk = pieces
        cumulative_decay = jnp.cumsum(l_blk, axis=1)
        block_final_state = cumulative_decay[:, -1:, :]
        relative = cumulative_decay[:, :, None, :] - cumulative_decay[:, None, :, :]
        decays = jnp.exp(jnp.where(lower_tri, relative, NEG_BIG))
        scores = jnp.einsum('htk,hsk,htsk->hts', query_block, key_block, decays, precision=HIGH_PRECISION)
        block_result = jnp.einsum('hts,hsv->htv', scores, value_block, precision=HIGH_PRECISION)
        block_result = block_result + jnp.einsum('dyr,dru->dyu', query_block * jnp.exp(cumulative_decay), carried_state, precision=HIGH_PRECISION)
        carried_state = jnp.exp(block_final_state[:, 0, :])[:, :, None] * carried_state + jnp.einsum('qfw,qfa->qwa', key_block * jnp.exp(block_final_state - cumulative_decay), value_block, precision=HIGH_PRECISION)
        return (carried_state, block_result)
    final_state, block_outs = lax.scan(advance, state_in, (blocks(query_heads), blocks(key_gate), blocks(v_heads), blocks(shrink_exponent)))
    return (jnp.moveaxis(block_outs, 0, 1).reshape(channel_group_count, length, v_heads.shape[-1]), final_state)

def to_heads(matrix, channel_group_count):
    length = matrix.shape[0]
    return matrix.astype(jnp.float32).reshape(length, channel_group_count, -1).transpose(1, 0, 2)

def retain_factors(retain_scores, retain_minimum, extra_shrink_spikes, channel_group_count):
    pre_act = to_heads(retain_scores, channel_group_count)
    floor_b = retain_minimum.reshape(channel_group_count, 1, -1)
    retain_factor = floor_b + (1.0 - floor_b) * jax.nn.sigmoid(pre_act)
    shrink_exponent = jnp.log(retain_factor) + extra_shrink_spikes[:, :, None]
    key_gate = (1.0 - floor_b) * jax.nn.sigmoid(-pre_act)
    return (key_gate, shrink_exponent)

def reverse_seq(tensor):
    return jnp.flip(tensor, axis=1)

def rounded(partial_value):
    return lax.optimization_barrier(partial_value.astype(jnp.bfloat16)).astype(jnp.float32)

def reference(probe_preactivations, rightward_retain_scores, leftward_retain_scores, payload_vectors, retain_minimum_bounds, extra_shrink_spikes, mixer_rescale_factor, mixer_emit_matrix, specialist_arriving_tokens, specialist_rescale_factor, routed_specialist_ids, routed_specialist_shares, specialist_switch_matrix, specialist_widen_matrix, specialist_shrink_matrix):
    query_heads = jax.nn.silu(to_heads(probe_preactivations, MIXER_STREAMS))
    v_heads = to_heads(payload_vectors, MIXER_STREAMS)
    rightward_seed, rightward_shrink_exponent = retain_factors(rightward_retain_scores, retain_minimum_bounds[0], extra_shrink_spikes, MIXER_STREAMS)
    leftward_seed, leftward_shrink_exponent = retain_factors(leftward_retain_scores, retain_minimum_bounds[1], extra_shrink_spikes, MIXER_STREAMS)
    zero_state = jnp.zeros((MIXER_STREAMS, DK, DV), jnp.float32)
    out_fwd, _ = recurrence(query_heads, rightward_seed, v_heads, rightward_shrink_exponent, zero_state)
    out_bwd, _ = recurrence(reverse_seq(query_heads), reverse_seq(leftward_seed), reverse_seq(v_heads), reverse_seq(leftward_shrink_exponent), zero_state)
    combined = out_fwd + reverse_seq(out_bwd)
    normed = combined * lax.rsqrt(lax.optimization_barrier(jnp.mean(combined * combined, axis=-1, keepdims=True)) + EPS)
    normed = normed * mixer_rescale_factor.reshape(MIXER_STREAMS, 1, DV)
    mixed_heads = normed.transpose(1, 0, 2).reshape(SEQ, D).astype(jnp.bfloat16)
    head_groups = mixed_heads.reshape(SEQ, N_TP, D // N_TP).transpose(1, 0, 2)
    weight_groups = mixer_emit_matrix.reshape(N_TP, D // N_TP, D)

    def add_group(running, operands):
        partial_value = jnp.dot(operands[0], operands[1], preferred_element_type=jnp.float32)
        return (running + rounded(partial_value), None)
    summed_a, _ = lax.scan(add_group, jnp.zeros((SEQ, D), jnp.float32), (head_groups, weight_groups))
    mixed_a = summed_a.astype(jnp.bfloat16)
    rows_f = specialist_arriving_tokens.astype(jnp.float32)
    normed_b = (rows_f * lax.rsqrt(lax.optimization_barrier(jnp.mean(rows_f * rows_f, axis=-1, keepdims=True)) + EPS) * specialist_rescale_factor).astype(jnp.bfloat16)
    flat_ids = routed_specialist_ids.reshape(-1).astype(jnp.int32)
    onehot = (flat_ids[:, None] == jnp.arange(EXPERTS, dtype=jnp.int32)[None, :]).astype(jnp.int32)
    ranking = lax.optimization_barrier(jnp.sum((jnp.cumsum(onehot, axis=0) - onehot) * onehot, axis=1)).astype(jnp.int32)
    slot_total = N_EP * CAP
    position = (flat_ids * slot_total + ranking).astype(jnp.int32)
    copy_row = (jnp.arange(flat_ids.shape[0], dtype=jnp.int32) // TOP_K).astype(jnp.int32)
    row_table = jnp.zeros((EXPERTS * slot_total,), jnp.int32).at[position].set(copy_row).reshape(EXPERTS, slot_total)
    live_table = jnp.zeros((EXPERTS * slot_total,), jnp.bfloat16).at[position].set(1.0).reshape(EXPERTS, slot_total)

    def run_expert(operands):
        gate_w, up_w, down_w, row_index, live_slot = operands
        gathered = normed_b[row_index] * live_slot[:, None]
        gate_out = jnp.dot(gathered, gate_w, preferred_element_type=jnp.float32)
        up_out = jnp.dot(gathered, up_w, preferred_element_type=jnp.float32)
        hidden = (jax.nn.silu(gate_out) * up_out).astype(jnp.bfloat16)
        hidden_groups = hidden.reshape(slot_total, N_TP, DE // N_TP).transpose(1, 0, 2)
        down_groups = down_w.reshape(N_TP, DE // N_TP, D)
        summed, _ = lax.scan(add_group, jnp.zeros((slot_total, D), jnp.float32), (hidden_groups, down_groups))
        return summed.astype(jnp.bfloat16)
    expert_out = lax.map(run_expert, (specialist_switch_matrix, specialist_widen_matrix, specialist_shrink_matrix, row_table, live_table))
    picked = expert_out.reshape(EXPERTS * slot_total, D)[position].astype(jnp.float32)
    picked = picked.reshape(ROWS_B, TOP_K, D)
    mixed_b = lax.optimization_barrier(jnp.sum(picked * routed_specialist_shares[:, :, None], axis=1)).astype(jnp.bfloat16)
    return (mixed_a, mixed_b)
```

```python
import jax
import jax.numpy as jnp
from jax import lax
from jax.experimental import pallas as pl
from jax.experimental.pallas import tpu as pltpu
from jax.sharding import PartitionSpec as P

DK = 128
CHUNK = 128
PAD = 16
EPS = 1e-06

NT = (((1,), (1,)), ((), ()))
TN = (((0,), (0,)), ((), ()))


def params(count):
    return pltpu.CompilerParams(dimension_semantics=("arbitrary",) * count)


def cost(flops, moved):
    return pl.CostEstimate(flops=flops, bytes_accessed=moved, transcendentals=0)


def dot(a, b, dims=(((1,), (0,)), ((), ()))):
    return lax.dot_general(a, b, dims, preferred_element_type=jnp.float32)


def split(x):
    high = x.astype(jnp.bfloat16)
    return high, (x - high.astype(jnp.float32)).astype(jnp.bfloat16)


def states_kernel(xf_ref, xb_ref, v_ref, bound_ref, spike_ref, cf_ref, eb_ref, state_ref):
    length, width = xf_ref.shape
    head = pl.program_id(0)
    bound_f = bound_ref[0:1, :]
    bound_b = bound_ref[1:2, :]
    spike = jnp.broadcast_to(spike_ref[pl.ds(head, 1), :], (width, length)).T
    row = lax.broadcasted_iota(jnp.int32, (CHUNK, CHUNK), 0)
    col = lax.broadcasted_iota(jnp.int32, (CHUNK, CHUNK), 1)
    tri = (row >= col).astype(jnp.bfloat16)
    carry_f = jnp.zeros((1, width), jnp.float32)
    carry_b = jnp.zeros((1, width), jnp.float32)
    keys_f, keys_b, cums_f = [], [], []
    for at in range(0, length, CHUNK):
        rows = slice(at, at + CHUNK)
        xf = xf_ref[rows, :].astype(jnp.float32)
        xb = xb_ref[rows, :].astype(jnp.float32)
        lf = jnp.log(bound_f + (1.0 - bound_f) * jax.nn.sigmoid(xf)) + spike[rows]
        lb = jnp.log(bound_b + (1.0 - bound_b) * jax.nn.sigmoid(xb)) + spike[rows]
        summed = dot(tri, jnp.concatenate([*split(lf), *split(lb)], axis=1))
        cf = carry_f + summed[:, :width] + summed[:, width : 2 * width]
        cb = carry_b + summed[:, 2 * width : 3 * width] + summed[:, 3 * width :]
        carry_f = cf[CHUNK - 1 :]
        carry_b = cb[CHUNK - 1 :]
        eb = cb - lb
        cf_ref[rows, :] = cf
        eb_ref[rows, :] = eb
        cums_f.append(cf)
        keys_f.append((1.0 - bound_f) * jax.nn.sigmoid(-xf))
        keys_b.append(((1.0 - bound_b) * jax.nn.sigmoid(-xb) * jnp.exp(eb)).astype(jnp.bfloat16))
    eb_ref[length:, :] = jnp.broadcast_to(carry_b, (8, width))
    keys_f = [(k * jnp.exp(carry_f - c)).astype(jnp.bfloat16) for k, c in zip(keys_f, cums_f)]
    v = v_ref[...]
    for way, (keys, total) in enumerate(((keys_f, carry_f), (keys_b, carry_b))):
        state = dot(v, jnp.concatenate(keys, axis=0), TN)
        high, low = split(jnp.broadcast_to(total, (PAD // 2, width)))
        state_ref[way, 0, :DK, :] = state.astype(jnp.bfloat16)
        state_ref[way, 0, DK:, :] = jnp.concatenate(
            [high.astype(jnp.float32), low.astype(jnp.float32)], axis=0
        ).astype(jnp.bfloat16)


def local_kernel(q_ref, xf_ref, xb_ref, v_ref, bound_ref, cf_ref, eb_ref, o_ref, qf_ref, qb_ref):
    length, width = xf_ref.shape
    bound_f = bound_ref[0:1, :]
    bound_b = bound_ref[1:2, :]
    row = lax.broadcasted_iota(jnp.int32, (CHUNK, CHUNK), 0)
    col = lax.broadcasted_iota(jnp.int32, (CHUNK, CHUNK), 1)
    total_b = eb_ref[length : length + 1, :]
    count = length // CHUNK
    bf = jnp.bfloat16
    later, outs = [], []
    state = None
    for c in range(count):
        at = c * CHUNK
        rows = slice(at, at + CHUNK)
        half = at + CHUNK // 2
        q = q_ref[rows, :].astype(jnp.float32)
        q = q * jax.nn.sigmoid(q)
        v = v_ref[rows, :]
        cf = cf_ref[rows, :]
        eb = eb_ref[rows, :]
        mid_f = cf_ref[half : half + 1, :]
        mid_b = eb_ref[half : half + 1, :]
        end_f = cf[CHUNK - 1 :]
        end_b = eb_ref[at + CHUNK : at + CHUNK + 1, :]
        kf = (1.0 - bound_f) * jax.nn.sigmoid(-xf_ref[rows, :].astype(jnp.float32))
        kb = (1.0 - bound_b) * jax.nn.sigmoid(-xb_ref[rows, :].astype(jnp.float32))
        q_f = q * jnp.exp(cf - mid_f)
        k_f = kf * jnp.exp(mid_f - cf)
        q_b = q * jnp.exp(mid_b - eb)
        k_b = kb * jnp.exp(eb - mid_b)
        scores = jnp.where(row >= col, dot(q_f.astype(bf), k_f.astype(bf), NT), 0.0)
        scores += jnp.where(row <= col, dot(q_b.astype(bf), k_b.astype(bf), NT), 0.0)
        out = dot(scores.astype(bf), v)
        qf_ref[rows, :] = (q_f * jnp.exp(mid_f)).astype(bf)
        qb_ref[rows, :] = (q_b * jnp.exp(total_b - mid_b)).astype(bf)
        base_f = cf_ref[at - 1 : at, :] if c else None
        if c:
            out += dot((q_f * jnp.exp(mid_f - base_f)).astype(bf), state.astype(bf), NT)
        if c < count - 1:
            gained = dot(v, (k_f * jnp.exp(end_f - mid_f)).astype(bf), TN)
            state = state * jnp.exp(end_f - base_f) + gained if c else gained
        start_b = eb[:1]
        into = (q_b * jnp.exp(end_b - mid_b)).astype(bf) if c < count - 1 else None
        gained_b = dot(v, (k_b * jnp.exp(mid_b - start_b)).astype(bf), TN) if c else None
        later.append((into, gained_b, end_b - start_b))
        outs.append(out)
    state = None
    for c in reversed(range(count)):
        into, gained_b, span = later[c]
        out = outs[c]
        if state is not None:
            out += dot(into, state.astype(bf), NT)
        o_ref[c * CHUNK : (c + 1) * CHUNK, :] = out
        if c:
            state = gained_b if state is None else state * jnp.exp(span) + gained_b


def join_kernel(place_ref, o_ref, qf_ref, qb_ref, all_ref, gain_ref, mixed_ref):
    place = place_ref[0]
    peers = all_ref.shape[0]
    width = o_ref.shape[1]

    def part(at, way):
        state = all_ref[at, way, 0, :DK, :].astype(jnp.float32)
        totals = all_ref[at, way, 0, DK:, :].astype(jnp.float32)
        return state, jnp.exp(totals[:1] + totals[PAD // 2 : PAD // 2 + 1])

    def forward(at, acc):
        state, decay = part(at, 0)
        return acc * decay + state

    def backward(k, acc):
        state, decay = part(peers - 1 - k, 1)
        return acc * decay + state

    zero = jnp.zeros((DK, width), jnp.float32)
    entry_f = lax.fori_loop(0, place, forward, zero).astype(jnp.bfloat16)
    entry_b = lax.fori_loop(0, peers - 1 - place, backward, zero).astype(jnp.bfloat16)
    out = o_ref[...] + dot(qf_ref[...], entry_f, NT) + dot(qb_ref[...], entry_b, NT)
    scale = lax.rsqrt(jnp.mean(out * out, axis=-1, keepdims=True) + EPS)
    mixed_ref[...] = (out * scale * gain_ref[...]).astype(jnp.bfloat16)


def partial_kernel(x_ref, w_ref, o_ref):
    o_ref[0] = dot(x_ref[...], w_ref[...]).astype(jnp.bfloat16)


def grouped(x, w, groups):
    rows, depth = x.shape
    cols = w.shape[1] // groups
    return pl.pallas_call(
        partial_kernel,
        grid=(groups,),
        in_specs=[
            pl.BlockSpec((rows, depth), lambda g: (0, 0)),
            pl.BlockSpec((depth, cols), lambda g: (0, g)),
        ],
        out_specs=pl.BlockSpec((1, rows, cols), lambda g: (g, 0, 0)),
        out_shape=jax.ShapeDtypeStruct((groups, rows, cols), jnp.bfloat16),
        compiler_params=params(1),
        cost_estimate=cost(2 * rows * depth * w.shape[1], 2 * (x.size + w.size + rows * w.shape[1])),
    )(x, w)


def per_device(
    probe_preactivations,
    rightward_retain_scores,
    leftward_retain_scores,
    payload_vectors,
    retain_minimum_bounds,
    extra_shrink_spikes,
    mixer_rescale_factor,
    mixer_emit_matrix,
    specialist_arriving_tokens,
    specialist_rescale_factor,
    routed_specialist_ids,
    routed_specialist_shares,
    specialist_switch_matrix,
    specialist_widen_matrix,
    specialist_shrink_matrix,
):
    peers = lax.axis_size("ep")
    groups = lax.axis_size("tp")
    length, width = probe_preactivations.shape
    heads = width // DK

    rows_b, features = specialist_arriving_tokens.shape
    picks = routed_specialist_ids.shape[1]
    capacity = 2 * rows_b * picks // peers
    slots = peers * capacity
    rows_f = specialist_arriving_tokens.astype(jnp.float32)
    normed_b = (
        rows_f
        * lax.rsqrt(jnp.mean(rows_f * rows_f, axis=-1, keepdims=True) + EPS)
        * specialist_rescale_factor
    ).astype(jnp.bfloat16)
    flat_ids = routed_specialist_ids.reshape(-1)
    number = jnp.arange(rows_b * picks, dtype=jnp.int32)
    same = (flat_ids[:, None] == flat_ids[None, :]) & (number[None, :] < number[:, None])
    ranking = jnp.sum(same.astype(jnp.int32), axis=1)
    slot_of = (flat_ids * capacity + ranking).reshape(rows_b, picks)
    slot_grid = jnp.arange(slots, dtype=jnp.int32)
    hits = slot_of[:, :, None] == slot_grid[None, None, :]
    pick_matrix = jnp.any(hits, axis=1).astype(jnp.bfloat16)
    share_matrix = jnp.sum(jnp.where(hits, routed_specialist_shares[:, :, None], 0.0), axis=1)
    outgoing = dot(pick_matrix, normed_b, TN).astype(jnp.bfloat16)
    arrived = lax.all_to_all(
        outgoing.reshape(peers, capacity, features), "ep", split_axis=0, concat_axis=0, tiled=True
    )

    tile = pl.BlockSpec((length, DK), lambda h: (0, h))
    tall = pl.BlockSpec((length + 8, DK), lambda h: (0, h))
    bound_tile = pl.BlockSpec((2, DK), lambda h: (0, h))
    wide = jax.ShapeDtypeStruct((length, width), jnp.float32)
    narrow = jax.ShapeDtypeStruct((length, width), jnp.bfloat16)
    cum_f, cum_b, states = pl.pallas_call(
        states_kernel,
        grid=(heads,),
        in_specs=[tile, tile, tile, bound_tile, pl.BlockSpec((heads, length), lambda h: (0, 0))],
        out_specs=[tile, tall, pl.BlockSpec((2, 1, DK + PAD, DK), lambda h: (0, h, 0, 0))],
        out_shape=[
            wide,
            jax.ShapeDtypeStruct((length + 8, width), jnp.float32),
            jax.ShapeDtypeStruct((2, heads, DK + PAD, DK), jnp.bfloat16),
        ],
        compiler_params=params(1),
        cost_estimate=cost(4 * 10**9, 16 * length * width),
    )(
        rightward_retain_scores,
        leftward_retain_scores,
        payload_vectors,
        retain_minimum_bounds,
        extra_shrink_spikes,
    )
    everything = lax.all_gather(states, "ep")
    local_out, query_f, query_b = pl.pallas_call(
        local_kernel,
        grid=(heads,),
        in_specs=[tile, tile, tile, tile, bound_tile, tile, tall],
        out_specs=[tile, tile, tile],
        out_shape=[wide, narrow, narrow],
        compiler_params=params(1),
        cost_estimate=cost(8 * 10**9, 24 * length * width),
    )(
        probe_preactivations,
        rightward_retain_scores,
        leftward_retain_scores,
        payload_vectors,
        retain_minimum_bounds,
        cum_f,
        cum_b,
    )

    arrived = arrived.reshape(slots, features)
    gate_out = dot(arrived, specialist_switch_matrix[0])
    up_out = dot(arrived, specialist_widen_matrix[0])
    hidden = (jax.nn.silu(gate_out) * up_out).astype(jnp.bfloat16)
    expert_part = grouped(hidden, specialist_shrink_matrix[0], groups)
    expert_total = lax.psum_scatter(expert_part, "tp", scatter_dimension=0, tiled=True)

    mixed_heads = pl.pallas_call(
        join_kernel,
        grid=(heads,),
        in_specs=[
            pl.BlockSpec(memory_space=pltpu.SMEM),
            tile,
            tile,
            tile,
            pl.BlockSpec((peers, 2, 1, DK + PAD, DK), lambda h: (0, 0, h, 0, 0)),
            pl.BlockSpec((1, DK), lambda h: (0, h)),
        ],
        out_specs=tile,
        out_shape=narrow,
        compiler_params=params(1),
        cost_estimate=cost(2 * 10**9, 10 * length * width),
    )(
        lax.axis_index("ep").reshape(1),
        local_out,
        query_f,
        query_b,
        everything,
        mixer_rescale_factor.reshape(1, -1),
    )
    mixer_part = grouped(mixed_heads, mixer_emit_matrix, groups)
    mixed_a = lax.psum_scatter(mixer_part, "tp", scatter_dimension=0, tiled=True)

    returned = lax.all_to_all(
        expert_total.reshape(peers, capacity, -1), "ep", split_axis=0, concat_axis=0, tiled=True
    ).reshape(slots, -1)
    share_high, share_low = split(share_matrix)
    mixed_b = (dot(share_high, returned) + dot(share_low, returned)).astype(jnp.bfloat16)
    return mixed_a.reshape(length, -1), mixed_b


def solution(mesh):
    in_specs = (
        P("ep", "tp"),
        P("ep", "tp"),
        P("ep", "tp"),
        P("ep", "tp"),
        P(None, "tp"),
        P("tp", "ep"),
        P("tp"),
        P("tp", None),
        P("ep", None),
        P(),
        P("ep", None),
        P("ep", None),
        P("ep", None, "tp"),
        P("ep", None, "tp"),
        P("ep", "tp", None),
    )
    out_specs = (P("ep", "tp"), P("ep", "tp"))
    return jax.shard_map(
        per_device, mesh=mesh, in_specs=in_specs, out_specs=out_specs, check_vma=False
    )
```

```python
import jax
import jax.numpy as jnp
from jax import lax
from jax.experimental import pallas as pl
from jax.experimental.pallas import tpu as pltpu
from jax.sharding import PartitionSpec as P

DK = 128
CHUNK = 128
EPS = 1e-06
MESH = pl.DeviceIdType.MESH
VMEM_LIMIT = 48 * 2**20

NT = (((1,), (1,)), ((), ()))
TN = (((0,), (0,)), ((), ()))


def cost(flops, moved):
    return pl.CostEstimate(flops=flops, bytes_accessed=moved, transcendentals=0)


def dot(a, b, dims=(((1,), (0,)), ((), ()))):
    return lax.dot_general(a, b, dims, preferred_element_type=jnp.float32)


def split(x):
    high = x.astype(jnp.bfloat16)
    return high, (x - high.astype(jnp.float32)).astype(jnp.bfloat16)


def states_of(xf_ref, xb_ref, v_ref, bound_ref, spike_ref, cf_ref, eb_ref, state_ref, total_ref):
    length, width = xf_ref.shape
    bound_f = bound_ref[0:1, :]
    bound_b = bound_ref[1:2, :]
    spike = jnp.broadcast_to(spike_ref[...], (width, length)).T
    row = lax.broadcasted_iota(jnp.int32, (CHUNK, CHUNK), 0)
    col = lax.broadcasted_iota(jnp.int32, (CHUNK, CHUNK), 1)
    tri = (row >= col).astype(jnp.bfloat16)
    carry_f = jnp.zeros((1, width), jnp.float32)
    carry_b = jnp.zeros((1, width), jnp.float32)
    keys_f, keys_b, cums_f = [], [], []
    for at in range(0, length, CHUNK):
        rows = slice(at, at + CHUNK)
        xf = xf_ref[rows, :].astype(jnp.float32)
        xb = xb_ref[rows, :].astype(jnp.float32)
        lf = jnp.log(bound_f + (1.0 - bound_f) * jax.nn.sigmoid(xf)) + spike[rows]
        lb = jnp.log(bound_b + (1.0 - bound_b) * jax.nn.sigmoid(xb)) + spike[rows]
        summed = dot(tri, jnp.concatenate([*split(lf), *split(lb)], axis=1))
        cf = carry_f + summed[:, :width] + summed[:, width : 2 * width]
        cb = carry_b + summed[:, 2 * width : 3 * width] + summed[:, 3 * width :]
        carry_f = cf[CHUNK - 1 :]
        carry_b = cb[CHUNK - 1 :]
        eb = cb - lb
        cf_ref[rows, :] = cf
        eb_ref[rows, :] = eb
        cums_f.append(cf)
        keys_f.append((1.0 - bound_f) * jax.nn.sigmoid(-xf))
        keys_b.append(((1.0 - bound_b) * jax.nn.sigmoid(-xb) * jnp.exp(eb)).astype(jnp.bfloat16))
    eb_ref[length:, :] = jnp.broadcast_to(carry_b, (8, width))
    keys_f = [(k * jnp.exp(carry_f - c)).astype(jnp.bfloat16) for k, c in zip(keys_f, cums_f)]
    v = v_ref[...]
    for way, (keys, total) in enumerate(((keys_f, carry_f), (keys_b, carry_b))):
        state_ref[way] = dot(v, jnp.concatenate(keys, axis=0), TN)
        total_ref[way] = jnp.broadcast_to(total, (8, width))


def local_of(q_ref, xf_ref, xb_ref, v_ref, bound_ref, cf_ref, eb_ref, o_ref, qf_ref, qb_ref):
    length, width = xf_ref.shape
    bound_f = bound_ref[0:1, :]
    bound_b = bound_ref[1:2, :]
    row = lax.broadcasted_iota(jnp.int32, (CHUNK, CHUNK), 0)
    col = lax.broadcasted_iota(jnp.int32, (CHUNK, CHUNK), 1)
    total_b = eb_ref[length : length + 1, :]
    count = length // CHUNK
    bf = jnp.bfloat16
    later, outs = [], []
    state = None
    for c in range(count):
        at = c * CHUNK
        rows = slice(at, at + CHUNK)
        half = at + CHUNK // 2
        q = q_ref[rows, :].astype(jnp.float32)
        q = q * jax.nn.sigmoid(q)
        v = v_ref[rows, :]
        cf = cf_ref[rows, :]
        eb = eb_ref[rows, :]
        mid_f = cf_ref[half : half + 1, :]
        mid_b = eb_ref[half : half + 1, :]
        end_f = cf[CHUNK - 1 :]
        end_b = eb_ref[at + CHUNK : at + CHUNK + 1, :]
        kf = (1.0 - bound_f) * jax.nn.sigmoid(-xf_ref[rows, :].astype(jnp.float32))
        kb = (1.0 - bound_b) * jax.nn.sigmoid(-xb_ref[rows, :].astype(jnp.float32))
        q_f = q * jnp.exp(cf - mid_f)
        k_f = kf * jnp.exp(mid_f - cf)
        q_b = q * jnp.exp(mid_b - eb)
        k_b = kb * jnp.exp(eb - mid_b)
        scores = jnp.where(row >= col, dot(q_f.astype(bf), k_f.astype(bf), NT), 0.0)
        scores += jnp.where(row <= col, dot(q_b.astype(bf), k_b.astype(bf), NT), 0.0)
        out = dot(scores.astype(bf), v)
        qf_ref[rows, :] = (q_f * jnp.exp(mid_f)).astype(bf)
        qb_ref[rows, :] = (q_b * jnp.exp(total_b - mid_b)).astype(bf)
        base_f = cf_ref[at - 1 : at, :] if c else None
        if c:
            out += dot((q_f * jnp.exp(mid_f - base_f)).astype(bf), state.astype(bf), NT)
        if c < count - 1:
            gained = dot(v, (k_f * jnp.exp(end_f - mid_f)).astype(bf), TN)
            state = state * jnp.exp(end_f - base_f) + gained if c else gained
        start_b = eb[:1]
        into = (q_b * jnp.exp(end_b - mid_b)).astype(bf) if c < count - 1 else None
        gained_b = dot(v, (k_b * jnp.exp(mid_b - start_b)).astype(bf), TN) if c else None
        later.append((into, gained_b, end_b - start_b))
        outs.append(out)
    state = None
    for c in reversed(range(count)):
        into, gained_b, span = later[c]
        out = outs[c]
        if state is not None:
            out += dot(into, state.astype(bf), NT)
        o_ref[c * CHUNK : (c + 1) * CHUNK, :] = out
        if c:
            state = gained_b if state is None else state * jnp.exp(span) + gained_b


def greet(axis):
    count = lax.axis_size(axis)
    me = lax.axis_index(axis)
    barrier = pltpu.get_barrier_semaphore()

    def one(k, carry):
        pl.semaphore_signal(barrier, inc=1, device_id={axis: lax.rem(me + k, count)}, device_id_type=MESH)
        return carry

    lax.fori_loop(1, count, one, 0)
    return count - 1


def sent(source, target, send, recv, axis, peer):
    return pltpu.make_async_remote_copy(
        src_ref=source,
        dst_ref=target,
        send_sem=send,
        recv_sem=recv,
        device_id={axis: peer},
        device_id_type=MESH,
    )


def head_kernel(
    q_ref,
    xf_ref,
    xb_ref,
    v_ref,
    bound_ref,
    spike_ref,
    gain_ref,
    outgoing_ref,
    arrived_ref,
    mixed_ref,
    cf_ref,
    eb_ref,
    local_ref,
    qf_ref,
    qb_ref,
    state_ref,
    total_ref,
    chain_out,
    chain_in,
    far_send,
    far_recv,
    near_send,
    near_recv,
    chain_send,
    chain_recv,
):
    peers, groups = lax.axis_size("ep"), lax.axis_size("tp")
    place, group = lax.axis_index("ep"), lax.axis_index("tp")
    heads = state_ref.shape[0]
    share = outgoing_ref.shape[2] // groups
    ours = pl.ds(pl.multiple_of(group * share, share), share)
    waits = greet("ep") + greet("tp")
    pl.semaphore_wait(pltpu.get_barrier_semaphore(), waits)

    far = []
    for k in range(1, peers):
        peer = lax.rem(place + k, peers)
        copy = sent(
            outgoing_ref.at[peer, :, ours],
            arrived_ref.at[place, :, ours],
            far_send.at[k - 1],
            far_recv.at[k - 1],
            "ep",
            peer,
        )
        copy.start()
        far.append(copy)
    arrived_ref[place] = outgoing_ref[place]

    def lanes(h):
        return pl.ds(pl.multiple_of(h * DK, DK), DK)

    def states_step(h, carry):
        at = lanes(h)
        states_of(
            xf_ref.at[:, at],
            xb_ref.at[:, at],
            v_ref.at[:, at],
            bound_ref.at[:, at],
            spike_ref.at[pl.ds(h, 1), :],
            cf_ref.at[h],
            eb_ref.at[h],
            state_ref.at[h],
            total_ref.at[h],
        )
        return carry

    lax.fori_loop(0, heads, states_step, 0)

    near = []
    for k in range(1, peers):
        far[k - 1].wait_recv()
        source = lax.rem(place + peers - k, peers)
        for j in range(1, groups):
            block = arrived_ref.at[source, :, ours]
            copy = sent(
                block,
                block,
                near_send.at[k - 1, j - 1],
                near_recv.at[k - 1, j - 1],
                "tp",
                lax.rem(group + j, groups),
            )
            copy.start()
            near.append(copy)

    def local_step(h, carry):
        at = lanes(h)
        local_of(
            q_ref.at[:, at],
            xf_ref.at[:, at],
            xb_ref.at[:, at],
            v_ref.at[:, at],
            bound_ref.at[:, at],
            cf_ref.at[h],
            eb_ref.at[h],
            local_ref.at[h],
            qf_ref.at[h],
            qb_ref.at[h],
        )
        return carry

    lax.fori_loop(0, heads, local_step, 0)

    def chain(way):
        first, last = (0, peers - 1) if way == 0 else (peers - 1, 0)
        to = lax.rem(place + (1 if way == 0 else peers - 1), peers)
        copy = sent(
            chain_out.at[way], chain_in.at[way], chain_send.at[way], chain_recv.at[way], "ep", to
        )

        def advance():
            @pl.when(place != first)
            def _():
                copy.wait_recv()

            @pl.when(place == first)
            def _():
                chain_in[way] = jnp.zeros(chain_in.shape[1:], jnp.bfloat16)

            @pl.when(place != last)
            def _():
                for h in range(heads):
                    decay = jnp.exp(total_ref[h, way][:1])
                    chain_out[way, h] = (
                        chain_in[way, h].astype(jnp.float32) * decay + state_ref[h, way]
                    ).astype(jnp.bfloat16)
                copy.start()

        def finish():
            @pl.when(place != last)
            def _():
                copy.wait_send()

        return advance, finish

    advance_f, finish_f = chain(0)
    advance_b, finish_b = chain(1)

    @pl.when(2 * place < peers)
    def _():
        advance_f()
        advance_b()

    @pl.when(2 * place >= peers)
    def _():
        advance_b()
        advance_f()

    def join_step(h, carry):
        at = lanes(h)
        out = local_ref[h] + dot(qf_ref[h], chain_in[0, h], NT) + dot(qb_ref[h], chain_in[1, h], NT)
        scale = lax.rsqrt(jnp.mean(out * out, axis=-1, keepdims=True) + EPS)
        mixed_ref[:, at] = (out * scale * gain_ref[:, at]).astype(jnp.bfloat16)
        return carry

    lax.fori_loop(0, heads, join_step, 0)
    finish_f()
    finish_b()
    for copy in far:
        copy.wait_send()
    for copy in near:
        copy.wait()


def tail_kernel(
    hidden_ref,
    down_ref,
    mixed_ref,
    emit_ref,
    high_ref,
    low_ref,
    out_a_ref,
    out_b_ref,
    part_b,
    got_b,
    part_a,
    got_a,
    total_b,
    returned,
    send_b,
    recv_b,
    send_a,
    recv_a,
    back_send,
    back_recv,
):
    peers, groups = lax.axis_size("ep"), lax.axis_size("tp")
    place, group = lax.axis_index("ep"), lax.axis_index("tp")
    cols = part_a.shape[2]
    waits = greet("ep") + greet("tp")
    pl.semaphore_wait(pltpu.get_barrier_semaphore(), waits)

    def scatter(x_ref, w_ref, part, got, send, recv):
        copies = []
        for k in range(1, groups + 1):
            peer = lax.rem(group + k, groups)
            at = pl.ds(pl.multiple_of(peer * cols, cols), cols)
            part[k - 1] = dot(x_ref[...], w_ref[:, at]).astype(jnp.bfloat16)
            if k < groups:
                copy = sent(part.at[k - 1], got.at[k - 1], send.at[k - 1], recv.at[k - 1], "tp", peer)
                copy.start()
                copies.append(copy)
        return copies

    def total(part, got, copies):
        for copy in copies:
            copy.wait_recv()
        value = part[groups - 1].astype(jnp.float32)
        for k in range(groups - 1):
            value += got[k].astype(jnp.float32)
        return value.astype(jnp.bfloat16)

    copies_b = scatter(hidden_ref, down_ref, part_b, got_b, send_b, recv_b)
    copies_a = scatter(mixed_ref, emit_ref, part_a, got_a, send_a, recv_a)
    total_b[...] = total(part_b, got_b, copies_b).reshape(total_b.shape)
    back = []
    for k in range(1, peers):
        peer = lax.rem(place + k, peers)
        copy = sent(
            total_b.at[peer], returned.at[place], back_send.at[k - 1], back_recv.at[k - 1], "ep", peer
        )
        copy.start()
        back.append(copy)
    returned[place] = total_b[place]
    out_a_ref[...] = total(part_a, got_a, copies_a)
    for copy in back:
        copy.wait_recv()
    rows = returned[...].reshape(-1, cols)
    out_b_ref[...] = (dot(high_ref[...], rows) + dot(low_ref[...], rows)).astype(jnp.bfloat16)
    for copy in copies_b + copies_a + back:
        copy.wait_send()


def per_device(
    probe_preactivations,
    rightward_retain_scores,
    leftward_retain_scores,
    payload_vectors,
    retain_minimum_bounds,
    extra_shrink_spikes,
    mixer_rescale_factor,
    mixer_emit_matrix,
    specialist_arriving_tokens,
    specialist_rescale_factor,
    routed_specialist_ids,
    routed_specialist_shares,
    specialist_switch_matrix,
    specialist_widen_matrix,
    specialist_shrink_matrix,
):
    peers = lax.axis_size("ep")
    groups = lax.axis_size("tp")
    length, width = probe_preactivations.shape
    heads = width // DK

    rows_b, features = specialist_arriving_tokens.shape
    picks = routed_specialist_ids.shape[1]
    capacity = 2 * rows_b * picks // peers
    slots = peers * capacity
    rows_f = specialist_arriving_tokens.astype(jnp.float32)
    normed_b = (
        rows_f
        * lax.rsqrt(jnp.mean(rows_f * rows_f, axis=-1, keepdims=True) + EPS)
        * specialist_rescale_factor
    ).astype(jnp.bfloat16)
    flat_ids = routed_specialist_ids.reshape(-1)
    number = jnp.arange(rows_b * picks, dtype=jnp.int32)
    same = (flat_ids[:, None] == flat_ids[None, :]) & (number[None, :] < number[:, None])
    ranking = jnp.sum(same.astype(jnp.int32), axis=1)
    slot_of = (flat_ids * capacity + ranking).reshape(rows_b, picks)
    slot_grid = jnp.arange(slots, dtype=jnp.int32)
    hits = slot_of[:, :, None] == slot_grid[None, None, :]
    pick_matrix = jnp.any(hits, axis=1).astype(jnp.bfloat16)
    share_matrix = jnp.sum(jnp.where(hits, routed_specialist_shares[:, :, None], 0.0), axis=1)
    outgoing = dot(pick_matrix, normed_b, TN).astype(jnp.bfloat16)
    vmem = pl.BlockSpec(memory_space=pltpu.VMEM)
    dma = pltpu.SemaphoreType.DMA
    bf, f32 = jnp.bfloat16, jnp.float32
    arrived, mixed_heads = pl.pallas_call(
        head_kernel,
        in_specs=[vmem] * 8,
        out_specs=[vmem] * 2,
        out_shape=[
            jax.ShapeDtypeStruct((peers, capacity, features), bf),
            jax.ShapeDtypeStruct((length, width), bf),
        ],
        scratch_shapes=[
            pltpu.VMEM((heads, length, DK), f32),
            pltpu.VMEM((heads, length + 8, DK), f32),
            pltpu.VMEM((heads, length, DK), f32),
            pltpu.VMEM((heads, length, DK), bf),
            pltpu.VMEM((heads, length, DK), bf),
            pltpu.VMEM((heads, 2, DK, DK), f32),
            pltpu.VMEM((heads, 2, 8, DK), f32),
            pltpu.VMEM((2, heads, DK, DK), bf),
            pltpu.VMEM((2, heads, DK, DK), bf),
            dma((peers - 1,)),
            dma((peers - 1,)),
            dma((peers - 1, groups - 1)),
            dma((peers - 1, groups - 1)),
            dma((2,)),
            dma((2,)),
        ],
        compiler_params=pltpu.CompilerParams(
            collective_id=0, has_side_effects=True, vmem_limit_bytes=VMEM_LIMIT
        ),
        cost_estimate=cost(2 * 10**10, 10**7),
    )(
        probe_preactivations,
        rightward_retain_scores,
        leftward_retain_scores,
        payload_vectors,
        retain_minimum_bounds,
        extra_shrink_spikes,
        mixer_rescale_factor.reshape(1, -1),
        outgoing.reshape(peers, capacity, features),
    )

    arrived = arrived.reshape(slots, features)
    gate_out = dot(arrived, specialist_switch_matrix[0])
    up_out = dot(arrived, specialist_widen_matrix[0])
    hidden = (jax.nn.silu(gate_out) * up_out).astype(bf)

    share_high, share_low = split(share_matrix)
    cols = features // groups
    cols_a = mixer_emit_matrix.shape[1] // groups
    return tuple(
        pl.pallas_call(
            tail_kernel,
            in_specs=[vmem] * 6,
            out_specs=[vmem] * 2,
            out_shape=[
                jax.ShapeDtypeStruct((length, cols_a), bf),
                jax.ShapeDtypeStruct((rows_b, cols), bf),
            ],
            scratch_shapes=[
                pltpu.VMEM((groups, slots, cols), bf),
                pltpu.VMEM((groups - 1, slots, cols), bf),
                pltpu.VMEM((groups, length, cols_a), bf),
                pltpu.VMEM((groups - 1, length, cols_a), bf),
                pltpu.VMEM((peers, capacity, cols), bf),
                pltpu.VMEM((peers, capacity, cols), bf),
                dma((groups - 1,)),
                dma((groups - 1,)),
                dma((groups - 1,)),
                dma((groups - 1,)),
                dma((peers - 1,)),
                dma((peers - 1,)),
            ],
            compiler_params=pltpu.CompilerParams(
                collective_id=1, has_side_effects=True, vmem_limit_bytes=VMEM_LIMIT
            ),
            cost_estimate=cost(2 * 10**10, 10**7),
        )(
            hidden,
            specialist_shrink_matrix[0],
            mixed_heads,
            mixer_emit_matrix,
            share_high,
            share_low,
        )
    )


def solution(mesh):
    in_specs = (
        P("ep", "tp"),
        P("ep", "tp"),
        P("ep", "tp"),
        P("ep", "tp"),
        P(None, "tp"),
        P("tp", "ep"),
        P("tp"),
        P("tp", None),
        P("ep", None),
        P(),
        P("ep", None),
        P("ep", None),
        P("ep", None, "tp"),
        P("ep", None, "tp"),
        P("ep", "tp", None),
    )
    out_specs = (P("ep", "tp"), P("ep", "tp"))
    return jax.shard_map(
        per_device, mesh=mesh, in_specs=in_specs, out_specs=out_specs, check_vma=False
    )
```

```python
import jax
import jax.numpy as jnp
from jax import lax
from jax.experimental import pallas as pl
from jax.experimental.pallas import tpu as pltpu
from jax.sharding import PartitionSpec as P

DK = 128
CHUNK = 128
EPS = 1e-06
MESH = pl.DeviceIdType.MESH
VMEM_LIMIT = 48 * 2**20

NT = (((1,), (1,)), ((), ()))
TN = (((0,), (0,)), ((), ()))


def cost(flops, moved):
    return pl.CostEstimate(flops=flops, bytes_accessed=moved, transcendentals=0)


def dot(a, b, dims=(((1,), (0,)), ((), ()))):
    return lax.dot_general(a, b, dims, preferred_element_type=jnp.float32)


def split(x):
    high = x.astype(jnp.bfloat16)
    return high, (x - high.astype(jnp.float32)).astype(jnp.bfloat16)


def states_of(xf_ref, xb_ref, v_ref, bound_ref, spike_ref, cf_ref, eb_ref, state_ref, total_ref):
    length, width = xf_ref.shape
    bound_f = bound_ref[0:1, :]
    bound_b = bound_ref[1:2, :]
    spike = jnp.broadcast_to(spike_ref[...], (width, length)).T
    row = lax.broadcasted_iota(jnp.int32, (CHUNK, CHUNK), 0)
    col = lax.broadcasted_iota(jnp.int32, (CHUNK, CHUNK), 1)
    tri = (row >= col).astype(jnp.bfloat16)
    carry_f = jnp.zeros((1, width), jnp.float32)
    carry_b = jnp.zeros((1, width), jnp.float32)
    keys_f, keys_b, cums_f = [], [], []
    for at in range(0, length, CHUNK):
        rows = slice(at, at + CHUNK)
        xf = xf_ref[rows, :].astype(jnp.float32)
        xb = xb_ref[rows, :].astype(jnp.float32)
        lf = jnp.log(bound_f + (1.0 - bound_f) * jax.nn.sigmoid(xf)) + spike[rows]
        lb = jnp.log(bound_b + (1.0 - bound_b) * jax.nn.sigmoid(xb)) + spike[rows]
        summed = dot(tri, jnp.concatenate([*split(lf), *split(lb)], axis=1))
        cf = carry_f + summed[:, :width] + summed[:, width : 2 * width]
        cb = carry_b + summed[:, 2 * width : 3 * width] + summed[:, 3 * width :]
        carry_f = cf[CHUNK - 1 :]
        carry_b = cb[CHUNK - 1 :]
        eb = cb - lb
        cf_ref[rows, :] = cf
        eb_ref[rows, :] = eb
        cums_f.append(cf)
        keys_f.append((1.0 - bound_f) * jax.nn.sigmoid(-xf))
        keys_b.append(((1.0 - bound_b) * jax.nn.sigmoid(-xb) * jnp.exp(eb)).astype(jnp.bfloat16))
    eb_ref[length:, :] = jnp.broadcast_to(carry_b, (8, width))
    keys_f = [(k * jnp.exp(carry_f - c)).astype(jnp.bfloat16) for k, c in zip(keys_f, cums_f)]
    v = v_ref[...]
    for way, (keys, total) in enumerate(((keys_f, carry_f), (keys_b, carry_b))):
        state_ref[way] = dot(v, jnp.concatenate(keys, axis=0), TN)
        total_ref[way] = jnp.broadcast_to(total, (8, width))


def local_of(q_ref, xf_ref, xb_ref, v_ref, bound_ref, cf_ref, eb_ref, o_ref, qf_ref, qb_ref):
    length, width = xf_ref.shape
    bound_f = bound_ref[0:1, :]
    bound_b = bound_ref[1:2, :]
    row = lax.broadcasted_iota(jnp.int32, (CHUNK, CHUNK), 0)
    col = lax.broadcasted_iota(jnp.int32, (CHUNK, CHUNK), 1)
    total_b = eb_ref[length : length + 1, :]
    count = length // CHUNK
    bf = jnp.bfloat16
    later, outs = [], []
    state = None
    for c in range(count):
        at = c * CHUNK
        rows = slice(at, at + CHUNK)
        half = at + CHUNK // 2
        q = q_ref[rows, :].astype(jnp.float32)
        q = q * jax.nn.sigmoid(q)
        v = v_ref[rows, :]
        cf = cf_ref[rows, :]
        eb = eb_ref[rows, :]
        mid_f = cf_ref[half : half + 1, :]
        mid_b = eb_ref[half : half + 1, :]
        end_f = cf[CHUNK - 1 :]
        end_b = eb_ref[at + CHUNK : at + CHUNK + 1, :]
        kf = (1.0 - bound_f) * jax.nn.sigmoid(-xf_ref[rows, :].astype(jnp.float32))
        kb = (1.0 - bound_b) * jax.nn.sigmoid(-xb_ref[rows, :].astype(jnp.float32))
        q_f = q * jnp.exp(cf - mid_f)
        k_f = kf * jnp.exp(mid_f - cf)
        q_b = q * jnp.exp(mid_b - eb)
        k_b = kb * jnp.exp(eb - mid_b)
        scores = jnp.where(row >= col, dot(q_f.astype(bf), k_f.astype(bf), NT), 0.0)
        scores += jnp.where(row <= col, dot(q_b.astype(bf), k_b.astype(bf), NT), 0.0)
        out = dot(scores.astype(bf), v)
        qf_ref[rows, :] = (q_f * jnp.exp(mid_f)).astype(bf)
        qb_ref[rows, :] = (q_b * jnp.exp(total_b - mid_b)).astype(bf)
        base_f = cf_ref[at - 1 : at, :] if c else None
        if c:
            out += dot((q_f * jnp.exp(mid_f - base_f)).astype(bf), state.astype(bf), NT)
        if c < count - 1:
            gained = dot(v, (k_f * jnp.exp(end_f - mid_f)).astype(bf), TN)
            state = state * jnp.exp(end_f - base_f) + gained if c else gained
        start_b = eb[:1]
        into = (q_b * jnp.exp(end_b - mid_b)).astype(bf) if c < count - 1 else None
        gained_b = dot(v, (k_b * jnp.exp(mid_b - start_b)).astype(bf), TN) if c else None
        later.append((into, gained_b, end_b - start_b))
        outs.append(out)
    state = None
    for c in reversed(range(count)):
        into, gained_b, span = later[c]
        out = outs[c]
        if state is not None:
            out += dot(into, state.astype(bf), NT)
        o_ref[c * CHUNK : (c + 1) * CHUNK, :] = out
        if c:
            state = gained_b if state is None else state * jnp.exp(span) + gained_b


def greet(axis):
    count = lax.axis_size(axis)
    me = lax.axis_index(axis)
    barrier = pltpu.get_barrier_semaphore()

    def one(k, carry):
        pl.semaphore_signal(barrier, inc=1, device_id={axis: lax.rem(me + k, count)}, device_id_type=MESH)
        return carry

    lax.fori_loop(1, count, one, 0)
    return count - 1


def sent(source, target, send, recv, axis, peer):
    return pltpu.make_async_remote_copy(
        src_ref=source,
        dst_ref=target,
        send_sem=send,
        recv_sem=recv,
        device_id={axis: peer},
        device_id_type=MESH,
    )


def head_kernel(
    q_ref,
    xf_ref,
    xb_ref,
    v_ref,
    bound_ref,
    spike_ref,
    gain_ref,
    outgoing_ref,
    arrived_ref,
    mixed_ref,
    cf_ref,
    eb_ref,
    local_ref,
    qf_ref,
    qb_ref,
    state_ref,
    total_ref,
    chain_out,
    chain_in,
    far_send,
    far_recv,
    near_send,
    near_recv,
    chain_send,
    chain_recv,
):
    peers, groups = lax.axis_size("ep"), lax.axis_size("tp")
    place, group = lax.axis_index("ep"), lax.axis_index("tp")
    heads = state_ref.shape[0]
    share = outgoing_ref.shape[2] // groups
    ours = pl.ds(pl.multiple_of(group * share, share), share)
    waits = greet("ep") + greet("tp")
    pl.semaphore_wait(pltpu.get_barrier_semaphore(), waits)

    far = []
    for k in range(1, peers):
        peer = lax.rem(place + k, peers)
        copy = sent(
            outgoing_ref.at[peer, :, ours],
            arrived_ref.at[place, :, ours],
            far_send.at[k - 1],
            far_recv.at[k - 1],
            "ep",
            peer,
        )
        copy.start()
        far.append(copy)
    arrived_ref[place] = outgoing_ref[place]

    def lanes(h):
        return pl.ds(pl.multiple_of(h * DK, DK), DK)

    def states_step(h, carry):
        at = lanes(h)
        states_of(
            xf_ref.at[:, at],
            xb_ref.at[:, at],
            v_ref.at[:, at],
            bound_ref.at[:, at],
            spike_ref.at[pl.ds(h, 1), :],
            cf_ref.at[h],
            eb_ref.at[h],
            state_ref.at[h],
            total_ref.at[h],
        )
        return carry

    lax.fori_loop(0, heads, states_step, 0)

    near = []
    for k in range(1, peers):
        far[k - 1].wait_recv()
        source = lax.rem(place + peers - k, peers)
        for j in range(1, groups):
            block = arrived_ref.at[source, :, ours]
            copy = sent(
                block,
                block,
                near_send.at[k - 1, j - 1],
                near_recv.at[k - 1, j - 1],
                "tp",
                lax.rem(group + j, groups),
            )
            copy.start()
            near.append(copy)

    def local_step(h, carry):
        at = lanes(h)
        local_of(
            q_ref.at[:, at],
            xf_ref.at[:, at],
            xb_ref.at[:, at],
            v_ref.at[:, at],
            bound_ref.at[:, at],
            cf_ref.at[h],
            eb_ref.at[h],
            local_ref.at[h],
            qf_ref.at[h],
            qb_ref.at[h],
        )
        return carry

    lax.fori_loop(0, heads, local_step, 0)

    def chain(way):
        first, last = (0, peers - 1) if way == 0 else (peers - 1, 0)
        to = lax.rem(place + (1 if way == 0 else peers - 1), peers)
        copy = sent(
            chain_out.at[way], chain_in.at[way], chain_send.at[way], chain_recv.at[way], "ep", to
        )

        def advance():
            @pl.when(place != first)
            def _():
                copy.wait_recv()

            @pl.when(place == first)
            def _():
                chain_in[way] = jnp.zeros(chain_in.shape[1:], jnp.bfloat16)

            @pl.when(place != last)
            def _():
                for h in range(heads):
                    decay = jnp.exp(total_ref[h, way][:1])
                    chain_out[way, h] = (
                        chain_in[way, h].astype(jnp.float32) * decay + state_ref[h, way]
                    ).astype(jnp.bfloat16)
                copy.start()

        def finish():
            @pl.when(place != last)
            def _():
                copy.wait_send()

        return advance, finish

    advance_f, finish_f = chain(0)
    advance_b, finish_b = chain(1)

    @pl.when(2 * place < peers)
    def _():
        advance_f()
        advance_b()

    @pl.when(2 * place >= peers)
    def _():
        advance_b()
        advance_f()

    def join_step(h, carry):
        at = lanes(h)
        out = local_ref[h] + dot(qf_ref[h], chain_in[0, h], NT) + dot(qb_ref[h], chain_in[1, h], NT)
        scale = lax.rsqrt(jnp.mean(out * out, axis=-1, keepdims=True) + EPS)
        mixed_ref[:, at] = (out * scale * gain_ref[:, at]).astype(jnp.bfloat16)
        return carry

    lax.fori_loop(0, heads, join_step, 0)
    finish_f()
    finish_b()
    for copy in far:
        copy.wait_send()
    for copy in near:
        copy.wait()


def tail_kernel(
    hidden_ref,
    down_ref,
    mixed_ref,
    emit_ref,
    high_ref,
    low_ref,
    out_a_ref,
    out_b_ref,
    part_b,
    got_b,
    part_a,
    got_a,
    total_b,
    returned,
    send_b,
    recv_b,
    send_a,
    recv_a,
    back_send,
    back_recv,
):
    peers, groups = lax.axis_size("ep"), lax.axis_size("tp")
    place, group = lax.axis_index("ep"), lax.axis_index("tp")
    cols = part_a.shape[2]
    waits = greet("ep") + greet("tp")
    pl.semaphore_wait(pltpu.get_barrier_semaphore(), waits)

    def scatter(x_ref, w_ref, part, got, send, recv):
        copies = []
        for k in range(1, groups + 1):
            peer = lax.rem(group + k, groups)
            at = pl.ds(pl.multiple_of(peer * cols, cols), cols)
            part[k - 1] = dot(x_ref[...], w_ref[:, at]).astype(jnp.bfloat16)
            if k < groups:
                copy = sent(part.at[k - 1], got.at[k - 1], send.at[k - 1], recv.at[k - 1], "tp", peer)
                copy.start()
                copies.append(copy)
        return copies

    def total(part, got, copies):
        for copy in copies:
            copy.wait_recv()
        value = part[groups - 1].astype(jnp.float32)
        for k in range(groups - 1):
            value += got[k].astype(jnp.float32)
        return value.astype(jnp.bfloat16)

    def block(x_ref, w_ref, peer):
        at = pl.ds(pl.multiple_of(peer * cols, cols), cols)
        return dot(x_ref[...], w_ref[:, at]).astype(jnp.bfloat16)

    side, line = lax.rem(group, 2), group // 2
    beside, across = 2 * line + 1 - side, 2 * (1 - line) + side
    corner = 2 * (1 - line) + 1 - side

    def plan(part, got, send, recv):
        half = part.shape[1] // 2
        top, low = pl.ds(0, half), pl.ds(half, half)

        def make(k, p, g, rows, peer):
            return sent(part.at[p, rows], got.at[g, rows], send.at[k], recv.at[k], "tp", peer)

        first = [
            make(0, 0, 1, top, beside),
            make(1, 0, 1, low, across),
            make(2, 1, 0, top, beside),
            make(3, 2, 0, low, across),
        ]
        second = [make(4, 2, 2, top, across), make(5, 1, 2, low, beside)]
        return first, second

    def forward(part, got, first, second):
        half = part.shape[1] // 2
        for copy, mine, p, rows in (
            (second[0], first[0], 2, pl.ds(0, half)),
            (second[1], first[1], 1, pl.ds(half, half)),
        ):
            mine.wait_recv()
            summed = part[p, rows].astype(jnp.float32) + got[1, rows].astype(jnp.float32)
            part[p, rows] = summed.astype(jnp.bfloat16)
            copy.start()

    def finish(part, got, first, second):
        for copy in first[2:] + second:
            copy.wait_recv()
        value = part[3].astype(jnp.float32) + got[0].astype(jnp.float32) + got[2].astype(jnp.float32)
        return value.astype(jnp.bfloat16)

    if groups == 4:
        plan_b = plan(part_b, got_b, send_b, recv_b)
        plan_a = plan(part_a, got_a, send_a, recv_a)
        part_b[0] = block(hidden_ref, down_ref, corner)
        plan_b[0][0].start()
        plan_b[0][1].start()
        part_b[1] = block(hidden_ref, down_ref, beside)
        plan_b[0][2].start()
        part_b[2] = block(hidden_ref, down_ref, across)
        plan_b[0][3].start()
        part_b[3] = block(hidden_ref, down_ref, group)
        for slot, peer in enumerate((corner, beside, across, group)):
            part_a[slot] = block(mixed_ref, emit_ref, peer)
        forward(part_b, got_b, *plan_b)
        for copy in plan_a[0]:
            copy.start()
        copies_b, copies_a = plan_b[0] + plan_b[1], plan_a[0] + plan_a[1]
        total_b[...] = finish(part_b, got_b, *plan_b).reshape(total_b.shape)
    else:
        copies_b = scatter(hidden_ref, down_ref, part_b, got_b, send_b, recv_b)
        copies_a = scatter(mixed_ref, emit_ref, part_a, got_a, send_a, recv_a)
        total_b[...] = total(part_b, got_b, copies_b).reshape(total_b.shape)
    back = []
    for k in range(1, peers):
        peer = lax.rem(place + k, peers)
        copy = sent(
            total_b.at[peer], returned.at[place], back_send.at[k - 1], back_recv.at[k - 1], "ep", peer
        )
        copy.start()
        back.append(copy)
    returned[place] = total_b[place]
    if groups == 4:
        forward(part_a, got_a, *plan_a)
        out_a_ref[...] = finish(part_a, got_a, *plan_a)
    else:
        out_a_ref[...] = total(part_a, got_a, copies_a)
    for copy in back:
        copy.wait_recv()
    rows = returned[...].reshape(-1, cols)
    out_b_ref[...] = (dot(high_ref[...], rows) + dot(low_ref[...], rows)).astype(jnp.bfloat16)
    for copy in copies_b + copies_a + back:
        copy.wait_send()


def per_device(
    probe_preactivations,
    rightward_retain_scores,
    leftward_retain_scores,
    payload_vectors,
    retain_minimum_bounds,
    extra_shrink_spikes,
    mixer_rescale_factor,
    mixer_emit_matrix,
    specialist_arriving_tokens,
    specialist_rescale_factor,
    routed_specialist_ids,
    routed_specialist_shares,
    specialist_switch_matrix,
    specialist_widen_matrix,
    specialist_shrink_matrix,
):
    peers = lax.axis_size("ep")
    groups = lax.axis_size("tp")
    length, width = probe_preactivations.shape
    heads = width // DK

    rows_b, features = specialist_arriving_tokens.shape
    picks = routed_specialist_ids.shape[1]
    capacity = 2 * rows_b * picks // peers
    slots = peers * capacity
    rows_f = specialist_arriving_tokens.astype(jnp.float32)
    normed_b = (
        rows_f
        * lax.rsqrt(jnp.mean(rows_f * rows_f, axis=-1, keepdims=True) + EPS)
        * specialist_rescale_factor
    ).astype(jnp.bfloat16)
    flat_ids = routed_specialist_ids.reshape(-1)
    number = jnp.arange(rows_b * picks, dtype=jnp.int32)
    same = (flat_ids[:, None] == flat_ids[None, :]) & (number[None, :] < number[:, None])
    ranking = jnp.sum(same.astype(jnp.int32), axis=1)
    slot_of = (flat_ids * capacity + ranking).reshape(rows_b, picks)
    slot_grid = jnp.arange(slots, dtype=jnp.int32)
    hits = slot_of[:, :, None] == slot_grid[None, None, :]
    pick_matrix = jnp.any(hits, axis=1).astype(jnp.bfloat16)
    share_matrix = jnp.sum(jnp.where(hits, routed_specialist_shares[:, :, None], 0.0), axis=1)
    outgoing = dot(pick_matrix, normed_b, TN).astype(jnp.bfloat16)
    vmem = pl.BlockSpec(memory_space=pltpu.VMEM)
    dma = pltpu.SemaphoreType.DMA
    bf, f32 = jnp.bfloat16, jnp.float32
    arrived, mixed_heads = pl.pallas_call(
        head_kernel,
        in_specs=[vmem] * 8,
        out_specs=[vmem] * 2,
        out_shape=[
            jax.ShapeDtypeStruct((peers, capacity, features), bf),
            jax.ShapeDtypeStruct((length, width), bf),
        ],
        scratch_shapes=[
            pltpu.VMEM((heads, length, DK), f32),
            pltpu.VMEM((heads, length + 8, DK), f32),
            pltpu.VMEM((heads, length, DK), f32),
            pltpu.VMEM((heads, length, DK), bf),
            pltpu.VMEM((heads, length, DK), bf),
            pltpu.VMEM((heads, 2, DK, DK), f32),
            pltpu.VMEM((heads, 2, 8, DK), f32),
            pltpu.VMEM((2, heads, DK, DK), bf),
            pltpu.VMEM((2, heads, DK, DK), bf),
            dma((peers - 1,)),
            dma((peers - 1,)),
            dma((peers - 1, groups - 1)),
            dma((peers - 1, groups - 1)),
            dma((2,)),
            dma((2,)),
        ],
        compiler_params=pltpu.CompilerParams(
            collective_id=0, has_side_effects=True, vmem_limit_bytes=VMEM_LIMIT
        ),
        cost_estimate=cost(2 * 10**10, 10**7),
    )(
        probe_preactivations,
        rightward_retain_scores,
        leftward_retain_scores,
        payload_vectors,
        retain_minimum_bounds,
        extra_shrink_spikes,
        mixer_rescale_factor.reshape(1, -1),
        outgoing.reshape(peers, capacity, features),
    )

    arrived = arrived.reshape(slots, features)
    gate_out = dot(arrived, specialist_switch_matrix[0])
    up_out = dot(arrived, specialist_widen_matrix[0])
    hidden = (jax.nn.silu(gate_out) * up_out).astype(bf)

    share_high, share_low = split(share_matrix)
    cols = features // groups
    cols_a = mixer_emit_matrix.shape[1] // groups
    return tuple(
        pl.pallas_call(
            tail_kernel,
            in_specs=[vmem] * 6,
            out_specs=[vmem] * 2,
            out_shape=[
                jax.ShapeDtypeStruct((length, cols_a), bf),
                jax.ShapeDtypeStruct((rows_b, cols), bf),
            ],
            scratch_shapes=[
                pltpu.VMEM((groups, slots, cols), bf),
                pltpu.VMEM((groups - 1, slots, cols), bf),
                pltpu.VMEM((groups, length, cols_a), bf),
                pltpu.VMEM((groups - 1, length, cols_a), bf),
                pltpu.VMEM((peers, capacity, cols), bf),
                pltpu.VMEM((peers, capacity, cols), bf),
                dma((max(groups - 1, 6),)),
                dma((max(groups - 1, 6),)),
                dma((max(groups - 1, 6),)),
                dma((max(groups - 1, 6),)),
                dma((peers - 1,)),
                dma((peers - 1,)),
            ],
            compiler_params=pltpu.CompilerParams(
                collective_id=1, has_side_effects=True, vmem_limit_bytes=VMEM_LIMIT
            ),
            cost_estimate=cost(2 * 10**10, 10**7),
        )(
            hidden,
            specialist_shrink_matrix[0],
            mixed_heads,
            mixer_emit_matrix,
            share_high,
            share_low,
        )
    )


def solution(mesh):
    in_specs = (
        P("ep", "tp"),
        P("ep", "tp"),
        P("ep", "tp"),
        P("ep", "tp"),
        P(None, "tp"),
        P("tp", "ep"),
        P("tp"),
        P("tp", None),
        P("ep", None),
        P(),
        P("ep", None),
        P("ep", None),
        P("ep", None, "tp"),
        P("ep", None, "tp"),
        P("ep", "tp", None),
    )
    out_specs = (P("ep", "tp"), P("ep", "tp"))
    return jax.shard_map(
        per_device, mesh=mesh, in_specs=in_specs, out_specs=out_specs, check_vma=False
    )
```
